32 devices in a mesh: ep: 8 (over z, y), tp: 4 (over x, core).
Axes of the slice: x: 2, y: 2, z: 4, core: 2. Of those that a mesh axis runs over, the one named last changes fastest.
Arguments:
- tokens: bfloat16 [128, 2048], P('ep'), may hold values from -6 to 6
- norm_gain: float32 [2048], replicated, may hold values from 0.1 to 1.9
- query_weight: bfloat16 [2048, 1024], P(None, 'tp'), may hold values from -0.21875 to 0.21875
- key_weight: bfloat16 [2048, 512], P(None, 'tp'), may hold values from -0.125 to 0.125
- value_weight: bfloat16 [2048, 512], P(None, 'tp'), may hold values from -0.125 to 0.125
- output_weight: bfloat16 [1024, 2048], P('tp'), may hold values from -0.1875 to 0.1875
- head_gain: float32 [128], replicated, may hold values from 0.1 to 1.9
- lambdas: float32 [8], P('tp'), may hold values from 0.3 to 0.8
- key_cache: bfloat16 [128, 1024, 4, 128], P('ep', None, 'tp')
- value_cache: bfloat16 [128, 1024, 4, 128], P('ep', None, 'tp'), may hold values from -6 to 6
- lengths: int32 [128], P('ep'), may hold values from 128 to 1024, as said below
- ffn_gain: float32 [2048], replicated, may hold values from 0.1 to 1.9
- routes: int32 [128, 4], P('ep'), may hold values from 0 to 7, all different within a row; in each aligned block of 16 rows (0 to 15, 16 to 31, ...) at most 16 rows name the same one
- route_weight: float32 [128, 4], P('ep'), may hold values from 0.1 to 1
- expert_gate: bfloat16 [8, 2048, 1024], P('ep', None, 'tp'), may hold values from -0.125 to 0.125
- expert_up: bfloat16 [8, 2048, 1024], P('ep', None, 'tp'), may hold values from -0.125 to 0.125
- expert_down: bfloat16 [8, 1024, 2048], P('ep', 'tp'), may hold values from -0.1875 to 0.1875
- dense_gate: bfloat16 [2048, 2048], P('tp'), may hold values from -0.125 to 0.125
- dense_up: bfloat16 [2048, 2048], P('tp'), may hold values from -0.125 to 0.125
- dense_down: bfloat16 [2048, 2048], P('tp'), may hold values from -0.1875 to 0.1875
- gate_vector: float32 [2048], P('tp')
Outputs:
- layer_out: bfloat16 [128, 2048], P('ep', 'tp')
The draws below stay inside these ranges and needn't reach their ends.
Inputs may be any that keep to these rules, and one draw needn't show every extreme that they name: `routes`: each row names 4 different experts. Among the rows of one index of ep no expert is named by more than 16 rows, a bound that some block reaches. `lengths`: some sequence has length 1024. Cached positions at or past a sequence's length are not read.
All inputs are finite; a program needn't handle non-finite values.
Results may differ from the reference program's by a relative error of at most 0.015.
The reference program's roundings to bfloat16 on the way count: a program that leaves them out, or rounds other values in their place, can miss the bound.
Values may be sent and summed in bfloat16 or wider, within the bound.
A program may use at most 128 MiB of HBM per device.

```python
import math
import jax
import jax.numpy as jnp
import numpy as np
from jax import lax

D = 2048
HEADS = 8
KV_HEADS = 4
DQK = 64
DV = 128
FFE = 1024
FFD = 2048
TOPK = 4
SEQ_DEV = 16
CACHE = 1024
SEQS = 128
EXPERTS = 8
CAP = 16
N_EP = 8
N_TP = 4


def draw_key_cache(key, part):
    normal_key = jax.random.fold_in(jax.random.fold_in(key, 11), 0)
    base_draw = jax.random.normal(normal_key, (SEQS, CACHE, KV_HEADS, 2 * DQK), jnp.float32)
    return base_draw.astype(jnp.bfloat16)


def draw_lengths(key, part):
    base_key, chosen_key = jax.random.split(jax.random.fold_in(key, 23))
    drawn = jax.random.randint(base_key, (SEQS,), CACHE // 8, CACHE + 1)
    chosen = jax.random.randint(chosen_key, (), 0, SEQS)
    return jnp.where(jnp.arange(SEQS) == chosen, CACHE, drawn).astype(jnp.int32)


def draw_gate_vector(key, part):
    inner_key = jax.random.fold_in(key, 37)
    rising = 1.0 + 3.0 * jnp.arange(FFD, dtype=jnp.float32) / FFD
    base_draw = jax.random.normal(inner_key, (FFD,), jnp.float32)
    return (base_draw * rising / math.sqrt(FFD)).astype(jnp.float32)


def with_spikes(entries, own_key, source, target, parts, factor):
    def block_of(position):
        return (jnp.arange(entries.shape[position]) // (entries.shape[position] // parts)).reshape((-1,) + (1,) * (entries.ndim - 1 - position))

    one_side = jax.random.permutation(own_key, parts)[block_of(target)]
    second = (block_of(target) + parts // 2) % parts
    return jnp.where((block_of(source) == one_side) | (block_of(source) == second), factor * entries, entries)


def levels(stream_key, dims, shards, smallest, top_value):
    level = 1.0
    for position, parts in shards:
        heights = jax.random.uniform(jax.random.fold_in(jax.random.fold_in(stream_key, 6), position), (parts,), jnp.float32, smallest / len(shards), top_value / len(shards))
        level = level * jnp.repeat(jnp.exp(heights), dims[position] // parts).reshape((-1,) + (1,) * (len(dims) - 1 - position))
    return level


def assign_block(own_key, own, number, rows, number_of, top, most, slope):
    ranking = jax.random.permutation(own_key, number_of)
    heavy_load, usual = shares(number_of, rows * top, most, slope, True), shares(number_of, rows * top, most, slope, False)
    places = jnp.arange(number_of)

    def named(sizes, rotation):
        used = int((sizes > 0).sum())
        fixed = max(1, used // 4)
        passed = fixed + (places - fixed + rotation * (used - fixed)) % max(1, number_of - fixed)
        return jnp.zeros((number_of,), jnp.int32).at[ranking[jnp.where(places < fixed, places, passed)]].set(jnp.asarray(sizes, jnp.int32))

    sizes = jnp.where(number % 4 == 0, named(heavy_load, number // 4), named(usual, number - number // 4 - 1))
    mixed = jax.random.permutation(jax.random.fold_in(own, 3), number_of)
    source_of, taker = mixed[0:number_of // 2 * 2:2], mixed[1:number_of // 2 * 2:2]
    room = jnp.minimum(sizes[source_of] - 1, most - sizes[taker]) // 2
    room = jnp.where((source_of == ranking[0]) | (taker == ranking[0]) | (sizes[taker] == 0), 0, jnp.maximum(room, 0))
    passed = jax.random.randint(jax.random.fold_in(own, 4), (number_of // 2,), 0, 1 << 20) % (room + 1)
    sizes = sizes.at[source_of].add(-passed).at[taker].add(passed)
    items = jnp.searchsorted(jnp.cumsum(sizes), jnp.arange(rows * top), side="right").astype(jnp.int32)
    listing = items.reshape(top, rows).T
    listing = listing[jax.random.permutation(jax.random.fold_in(own, 1), rows)]
    rotation = jax.random.randint(jax.random.fold_in(own, 2), (rows, 1), 0, top)
    return jnp.take_along_axis(listing, (jnp.arange(top)[None, :] + rotation) % top, axis=1)


def shares(count, total, bound, slope, full):
    loads = [(1 << 20) // math.isqrt(standing ** slope) + 1 for standing in range(1, count + 1)]
    largest = bound if full else min(bound, max(-(-total // count), total * loads[0] // sum(loads)))
    least = 1 if total - largest >= count - 1 else 0
    holding, surplus = [largest] + [least] * (count - 1), total - largest - least * (count - 1)
    while surplus > 0:
        candidates = [i for i in range(1, count) if holding[i] < largest] or [i for i in range(1, count) if holding[i] < bound]
        pool, left = sum([loads[i] for i in candidates]), surplus
        for i in candidates:
            addition = min(bound - holding[i], max(1, left * loads[i] // pool), surplus)
            holding[i] = holding[i] + addition
            surplus = surplus - addition
    return np.array(holding)


def gaussian(key, dims, width, reach, shards=(), held_as=jnp.bfloat16):
    values = jax.random.normal(key, dims, jnp.float32) * width
    if len(shards) > 0:
        values = levels(key, dims, shards, -0.22, 0.18) * values
    return jnp.clip(values, min=-reach, max=reach).astype(held_as)


def gaussian_with(stream_key, shape, width, limit, cuts, heavy, kind=jnp.bfloat16):
    values = width * jax.random.normal(stream_key, shape, jnp.float32)
    if cuts:
        values = values * levels(stream_key, shape, cuts, -0.22, 0.18)
    return jnp.clip(with_spikes(values, jax.random.fold_in(stream_key, 3), *heavy), -limit, limit).astype(kind)


def setup_inputs(seed: int = 0) -> dict:
    key_of = jax.random.split(jax.random.key(seed), 22)
    tokens = gaussian(key_of[0], (SEQS, D), 1.0, 6.0, ((0, 8),))
    norm_gain = jnp.clip(1.0 + 0.18 * jax.random.normal(key_of[1], (D,), jnp.float32), 0.1, 1.9)
    query_weight = gaussian(key_of[2], (D, HEADS * 2 * DQK), (D // 3) ** -0.5, 0.21875, ((1, 4),))
    key_weight = gaussian(key_of[3], (D, KV_HEADS * 2 * DQK), D ** -0.5, 0.125, ((1, 4),))
    value_weight = gaussian(key_of[4], (D, KV_HEADS * DV), D ** -0.5, 0.125, ((1, 4),))
    output_weight = gaussian(key_of[5], (HEADS * DV, D), (HEADS * DV) ** -0.5, 0.1875, ((0, 4),))
    head_gain = jnp.clip(1.0 + 0.18 * jax.random.normal(key_of[6], (DV,), jnp.float32), 0.1, 1.9)
    lambdas = jnp.clip(0.3 + 0.5 * jax.random.uniform(key_of[7], (HEADS,), jnp.float32) ** levels(key_of[7], (HEADS,), ((0, 4),), -0.2, 0.2), 0.3, 0.8)
    key_cache = draw_key_cache(jax.random.fold_in(key_of[21], 71), 0)
    value_cache = gaussian(key_of[9], (SEQS, CACHE, KV_HEADS, DV), 1.0, 6.0, ((0, 8), (2, 4)))
    lengths = draw_lengths(jax.random.fold_in(key_of[21], 71), 0)
    ffn_gain = jnp.clip(1.0 + 0.18 * jax.random.normal(key_of[11], (D,), jnp.float32), 0.1, 1.9)
    routes_keys = jax.random.split(jax.random.fold_in(key_of[12], 1), SEQS // SEQ_DEV)
    routes_turns = jax.random.permutation(jax.random.fold_in(key_of[12], 3), SEQS // SEQ_DEV)
    routes = jax.vmap(lambda own, number: assign_block(jax.random.fold_in(key_of[12], 2), own, number, SEQ_DEV, EXPERTS, TOPK, CAP, 2))(routes_keys, routes_turns).reshape((SEQS, TOPK))
    route_weight = jnp.clip(0.1 + 0.9 * jax.random.uniform(key_of[13], (SEQS, TOPK), jnp.float32) ** levels(key_of[13], (SEQS, TOPK), ((0, 8),), -0.2, 0.2), 0.1, 1.0)
    expert_gate = gaussian(key_of[14], (EXPERTS, D, FFE), D ** -0.5, 0.125, ((0, 8), (2, 4)))
    expert_up = gaussian(key_of[15], (EXPERTS, D, FFE), D ** -0.5, 0.125, ((0, 8), (2, 4)))
    expert_down = gaussian(key_of[16], (EXPERTS, FFE, D), FFE ** -0.5, 0.1875, ((0, 8), (1, 4)))
    dense_gate = gaussian(key_of[17], (FFD, D), D ** -0.5, 0.125, ((0, 4),))
    dense_up = gaussian(key_of[18], (FFD, D), D ** -0.5, 0.125, ((0, 4),))
    dense_down = gaussian_with(key_of[19], (FFD, D), FFD ** -0.5, 0.1875, ((0, 4),), (0, 1, 4, 2.0))
    gate_vector = draw_gate_vector(jax.random.fold_in(key_of[21], 71), 0)
    return {"tokens": tokens, "norm_gain": norm_gain, "query_weight": query_weight, "key_weight": key_weight, "value_weight": value_weight, "output_weight": output_weight, "head_gain": head_gain, "lambdas": lambdas, "key_cache": key_cache, "value_cache": value_cache, "lengths": lengths, "ffn_gain": ffn_gain, "routes": routes, "route_weight": route_weight, "expert_gate": expert_gate, "expert_up": expert_up, "expert_down": expert_down, "dense_gate": dense_gate, "dense_up": dense_up, "dense_down": dense_down, "gate_vector": gate_vector}


epsilon = 1e-06

def rms_scale(values, gain):
    return values * lax.rsqrt(lax.optimization_barrier(jnp.mean(values * values, axis=-1, keepdims=True)) + epsilon) * gain

def diff_attend(queries, new_key, new_value, key_rows, value_rows, length, lambda_grid):
    score_scale = DQK ** (-0.5)
    query_wide = queries.astype(jnp.float32)
    cache_scores = jnp.einsum('kgmd,ckmd->kgmc', query_wide, key_rows.astype(jnp.float32)) * score_scale
    own_score = jnp.einsum('kgmd,kmd->kgm', query_wide, new_key.astype(jnp.float32)) * score_scale
    live_mask = jnp.arange(CACHE) < length
    cache_scores = jnp.where(live_mask, cache_scores, -jnp.inf)
    top_score = jnp.maximum(lax.optimization_barrier(jnp.max(cache_scores, axis=-1)), own_score)
    cache_exp = jnp.exp(cache_scores - top_score[..., None])
    own_exp = jnp.exp(own_score - top_score)
    totals = lax.optimization_barrier(jnp.sum(cache_exp, axis=-1)) + own_exp
    cache_prob = cache_exp / totals[..., None]
    own_prob = own_exp / totals
    cache_weight = (cache_prob[:, :, 0] - lambda_grid[..., None] * cache_prob[:, :, 1]).astype(jnp.bfloat16)
    own_weight = (own_prob[:, :, 0] - lambda_grid * own_prob[:, :, 1]).astype(jnp.bfloat16)
    mixture = jnp.einsum('kgc,ckv->kgv', cache_weight.astype(jnp.float32), value_rows.astype(jnp.float32))
    return mixture + own_weight.astype(jnp.float32)[..., None] * new_value.astype(jnp.float32)[:, None, :]

def reference(tokens, norm_gain, query_weight, key_weight, value_weight, output_weight, head_gain, lambdas, key_cache, value_cache, lengths, ffn_gain, routes, route_weight, expert_gate, expert_up, expert_down, dense_gate, dense_up, dense_down, gate_vector):
    group_size = HEADS // KV_HEADS
    tokens_wide = tokens.astype(jnp.float32)
    normed = rms_scale(tokens_wide, norm_gain).astype(jnp.bfloat16)
    queries = jnp.dot(normed, query_weight, preferred_element_type=jnp.float32).astype(jnp.bfloat16)
    new_keys = jnp.dot(normed, key_weight, preferred_element_type=jnp.float32).astype(jnp.bfloat16)
    new_values = jnp.dot(normed, value_weight, preferred_element_type=jnp.float32).astype(jnp.bfloat16)
    queries = queries.reshape(SEQS, KV_HEADS, group_size, 2, DQK)
    new_keys = new_keys.reshape(SEQS, KV_HEADS, 2, DQK)
    new_values = new_values.reshape(SEQS, KV_HEADS, DV)
    lambda_grid = lambdas.reshape(KV_HEADS, group_size)

    def one_sequence(inputs):
        seq_query, seq_key, seq_value, seq_keys, seq_values, seq_length = inputs
        return diff_attend(seq_query, seq_key, seq_value, seq_keys.reshape(CACHE, KV_HEADS, 2, DQK), seq_values, seq_length, lambda_grid)
    mixture = lax.map(one_sequence, (queries, new_keys, new_values, key_cache, value_cache, lengths))
    head_rows = rms_scale(mixture, head_gain).astype(jnp.bfloat16).reshape(SEQS, HEADS * DV)
    block_rows = HEADS * DV // N_TP
    attention = jnp.zeros((SEQS, D), jnp.float32)
    for quarter in range(N_TP):
        partial_value = jnp.dot(head_rows[:, quarter * block_rows:(quarter + 1) * block_rows], output_weight[quarter * block_rows:(quarter + 1) * block_rows], preferred_element_type=jnp.float32)
        attention = attention + lax.optimization_barrier(partial_value.astype(jnp.bfloat16)).astype(jnp.float32)
    residual = tokens_wide + attention
    ffn_in = rms_scale(residual, ffn_gain).astype(jnp.bfloat16)
    gate_pre = jnp.dot(ffn_in, dense_gate.T, preferred_element_type=jnp.float32)
    up_proj = jnp.dot(ffn_in, dense_up.T, preferred_element_type=jnp.float32)
    dense_hidden = (jax.nn.silu(gate_pre) * up_proj).astype(jnp.bfloat16)
    gate_logit = lax.optimization_barrier(jnp.sum(dense_hidden.astype(jnp.float32) * gate_vector, axis=-1))
    dense_sum = jnp.dot(dense_hidden, dense_down, preferred_element_type=jnp.float32)
    dense_out = jax.nn.sigmoid(gate_logit)[:, None] * dense_sum
    pair_expert = routes.reshape(-1).astype(jnp.int32)
    onehot = (pair_expert[:, None] == jnp.arange(EXPERTS, dtype=jnp.int32)[None, :]).astype(jnp.int32)
    running = jnp.cumsum(onehot.reshape(N_EP, SEQ_DEV * TOPK, EXPERTS), axis=1).reshape(SEQS * TOPK, EXPERTS)
    slot_rank = lax.optimization_barrier(jnp.sum(running * onehot, axis=1)) - 1
    group_index = jnp.arange(SEQS * TOPK, dtype=jnp.int32) // (SEQ_DEV * TOPK)
    column = (group_index * CAP + slot_rank).astype(jnp.int32)
    token_of_pair = jnp.arange(SEQS * TOPK, dtype=jnp.int32) // TOPK
    buffer = jnp.zeros((EXPERTS, N_EP * CAP, D), jnp.bfloat16).at[pair_expert, column].set(ffn_in[token_of_pair])

    def expert_apply(inputs):
        row_block, w_gate, w_up, w_down = inputs
        expert_pre = jnp.dot(row_block, w_gate, preferred_element_type=jnp.float32)
        expert_upper = jnp.dot(row_block, w_up, preferred_element_type=jnp.float32)
        expert_hidden = (jax.nn.silu(expert_pre) * expert_upper).astype(jnp.bfloat16)
        quarter_width = FFE // N_TP
        summed = jnp.zeros((row_block.shape[0], D), jnp.float32)
        for quarter in range(N_TP):
            partial_value = jnp.dot(expert_hidden[:, quarter * quarter_width:(quarter + 1) * quarter_width], w_down[quarter * quarter_width:(quarter + 1) * quarter_width], preferred_element_type=jnp.float32)
            summed = summed + lax.optimization_barrier(partial_value.astype(jnp.bfloat16)).astype(jnp.float32)
        return summed.astype(jnp.bfloat16)
    expert_rows = lax.map(expert_apply, (buffer, expert_gate, expert_up, expert_down))
    picked = expert_rows[pair_expert, column].reshape(SEQS, TOPK, D).astype(jnp.float32)
    expert_mix = lax.optimization_barrier(jnp.sum(picked * route_weight[:, :, None], axis=1))
    return (residual + expert_mix + dense_out).astype(jnp.bfloat16)
```

```python
import functools

import jax
import jax.numpy as jnp
from jax import lax
from jax.experimental import pallas as pl
from jax.experimental.pallas import tpu as pltpu
from jax.sharding import PartitionSpec as P

HEADS = 8
KV_HEADS = 4
DQK = 64
DV = 128
TOPK = 4
SEQ_CHUNK = 4

epsilon = 1e-06
F32 = jnp.float32
BF16 = jnp.bfloat16
MESH = pl.DeviceIdType.MESH


def rms_scale(values, gain):
    return values * lax.rsqrt(jnp.mean(values * values, axis=-1, keepdims=True) + epsilon) * gain


def silu(v):
    return v / (1.0 + jnp.exp(-v))


def dot(a, b):
    return jnp.dot(a, b, preferred_element_type=F32)


def dot_nt(a, b):
    return lax.dot_general(a, b, (((1,), (1,)), ((), ())), preferred_element_type=F32)


def layer_kernel(
    n_ep, n_tp,
    lengths_h, lambdas_h,
    tokens_h, norm_gain_h, head_gain_h, ffn_gain_h, gate_vector_h, routes_h, weight_h,
    wq, wk, wv, wo, key_cache, value_cache, wg, wu, wd, dg, du, dd,
    out,
    lengths, lambdas, tokens, norm_gain, head_gain, ffn_gain, gate_vector, routes_t, weight_t,
    wq_v, wk_v, wv_v, wo_v, key_v, value_v, wg_v, wu_v, wd_v, dg_v, du_v, dd_v,
    q_rows, k_rows, v_rows, mix,
    ar_send, ar_recv, residual, gathered,
    d_send, d_recv, l_send, l_recv,
    p_send, n_recv, x_send, x_recv, e_send, e_recv,
    small_sem, load_sem, cache_sem,
    ar_ss, ar_rs, ag_ss, ag_rs, fw_ss, fw_rs, ds_ss, ds_rs, lg_ss, lg_rs, p_ss, p_rs, x_ss, x_rs, e_ss, e_rs,
):
    me = lax.axis_index("ep")
    mt = lax.axis_index("tp")
    n_seq, width = tokens.shape
    cache_len = key_cache.shape[1]
    cols = width // n_tp
    half = width // 2
    side = lax.rem(mt, 2)
    partner = mt + 1 - 2 * side
    far = mt // 2
    n_far = n_tp // 2
    inner = lax.rem(me, 2)
    across = me + 1 - 2 * inner
    outer = me // 2
    n_outer = n_ep // 2

    def ascending(k):
        return k + jnp.where(k >= outer, 1, 0)

    def descending(k):
        v = n_outer - 1 - k
        return v - jnp.where(v <= outer, 1, 0)

    def near_first(k):
        return jnp.where(2 * outer < n_outer, ascending(k), descending(k))

    def far_first(k):
        return jnp.where(2 * outer < n_outer, descending(k), ascending(k))

    def group_at(n):
        k = n // 2
        o = jnp.where(k < n_outer - 1, far_first(k), outer)
        return 2 * o + jnp.where(lax.rem(n, 2) == 0, 1 - inner, inner)

    def load(src, dst, sem):
        copy = pltpu.make_async_copy(src, dst, sem)
        copy.start()
        return copy

    small = [
        load(src, dst, small_sem.at[i]) for i, (src, dst) in enumerate((
            (tokens_h, tokens), (norm_gain_h, norm_gain), (lambdas_h, lambdas), (lengths_h, lengths),
            (head_gain_h, head_gain), (ffn_gain_h, ffn_gain), (gate_vector_h, gate_vector),
            (routes_h, routes_t), (weight_h, weight_t),
        ))
    ]
    first = [load(wq, wq_v, load_sem.at[0]), load(wk, wk_v, load_sem.at[1]), load(wv, wv_v, load_sem.at[2])]
    n_chunk = n_seq // SEQ_CHUNK

    def cache_copies(i):
        rows = pl.ds(i * SEQ_CHUNK, SEQ_CHUNK)
        return (
            pltpu.make_async_copy(key_cache.at[rows], key_v.at[rows], cache_sem.at[2 * i]),
            pltpu.make_async_copy(value_cache.at[rows], value_v.at[rows], cache_sem.at[2 * i + 1]),
        )

    def start_cache(i):
        for copy in cache_copies(i):
            copy.start()

    start_cache(0)
    barrier = pltpu.get_barrier_semaphore()
    for d in range(1, n_tp):
        pl.semaphore_signal(barrier, inc=1, device_id={"tp": lax.rem(mt + d, n_tp)}, device_id_type=MESH)

    @pl.loop(1, n_ep)
    def _(d):
        pl.semaphore_signal(barrier, inc=1, device_id={"ep": lax.rem(me + d, n_ep)}, device_id_type=MESH)

    for copy in small[:2]:
        copy.wait()
    wide = tokens[...].astype(F32)
    normed = rms_scale(wide, norm_gain[...]).astype(BF16)
    first[0].wait()
    for i in range(1, n_chunk):
        start_cache(i)
    wo_copy = load(wo, wo_v, load_sem.at[3])
    for copy in first[1:]:
        copy.wait()
    for copy in small[2:4]:
        copy.wait()
    q = dot(normed, wq_v[...]).astype(BF16).astype(F32)
    k_rows[:, 0, :] = dot(normed, wk_v[...]).astype(BF16).astype(F32)
    v_rows[:, 0, :] = dot(normed, wv_v[...]).astype(BF16).astype(F32)
    group = q.shape[1] // (2 * DQK)
    lane = lax.broadcasted_iota(jnp.int32, (n_seq, 2 * DQK), 1)
    q_rows[...] = jnp.zeros_like(q_rows)
    for h in range(group):
        qh = q[:, h * 2 * DQK:(h + 1) * 2 * DQK]
        q_rows[:, h, :] = jnp.where(lane < DQK, qh, 0.0)
        q_rows[:, 4 + h, :] = jnp.where(lane >= DQK, qh, 0.0)
    row_id = lax.broadcasted_iota(jnp.int32, (8, 1), 0)
    lam = jnp.zeros((8, 1), F32)
    for h in range(group):
        lam = jnp.where(row_id == h, lambdas[h], lam)
    position = lax.broadcasted_iota(jnp.int32, (8, cache_len), 1)
    scale = DQK ** (-0.5)

    @pl.loop(0, n_chunk)
    def _(i):
        for copy in cache_copies(i):
            copy.wait()
        seqs = [i * SEQ_CHUNK + j for j in range(SEQ_CHUNK)]
        qs = [q_rows[n] for n in seqs]
        raw = [dot_nt(qn.astype(BF16), key_v[n]) for qn, n in zip(qs, seqs)]
        own = [jnp.sum(qn * k_rows[n], axis=-1, keepdims=True) * scale for qn, n in zip(qs, seqs)]
        scores = [jnp.where(position < lengths[n], r * scale, -jnp.inf) for r, n in zip(raw, seqs)]
        top = [jnp.maximum(jnp.max(r, axis=-1, keepdims=True), o) for r, o in zip(scores, own)]
        e = [jnp.exp(r - t) for r, t in zip(scores, top)]
        own_e = [jnp.exp(o - t) for o, t in zip(own, top)]
        inv = [1.0 / (jnp.sum(en, axis=-1, keepdims=True) + o) for en, o in zip(e, own_e)]
        p = [en * v for en, v in zip(e, inv)]
        po = [jnp.broadcast_to(o * v, (8, DV)) for o, v in zip(own_e, inv)]
        w = [(pn - lam * pltpu.roll(pn, 4, 0)).astype(BF16) for pn in p]
        own_w = [(pn - lam * pltpu.roll(pn, 4, 0)).astype(BF16).astype(F32) for pn in po]
        mixed = [dot(wn, value_v[n]) + ow * v_rows[n] for wn, ow, n in zip(w, own_w, seqs)]
        for n, m in zip(seqs, mixed):
            mix[n] = m

    dense_in = [load(dg, dg_v, load_sem.at[4]), load(du, du_v, load_sem.at[5])]
    dense_out_copies = [load(dd.at[:, pl.ds(j * cols, cols)], dd_v.at[j], load_sem.at[8 + j]) for j in range(n_tp)]
    expert_in = [load(wg, wg_v, load_sem.at[6]), load(wu, wu_v, load_sem.at[7])]
    expert_out = [load(wd.at[:, pl.ds(j * cols, cols)], wd_v.at[j], load_sem.at[8 + n_tp + j]) for j in range(n_tp)]

    for copy in small[4:]:
        copy.wait()
    heads = [rms_scale(mix[:, h, :], head_gain[...]).astype(BF16) for h in range(group)]
    wo_copy.wait()
    partial = dot(heads[0], wo_v[0:DV, :])
    for h in range(1, group):
        partial = partial + dot(heads[h], wo_v[h * DV:(h + 1) * DV, :])
    ar_send[...] = partial.astype(BF16)

    pl.semaphore_wait(barrier, n_tp - 1 + n_ep - 1)

    def ar_copy(d):
        peer = lax.rem(mt + d, n_tp)
        return pltpu.make_async_remote_copy(
            ar_send, ar_recv.at[mt], ar_ss.at[0], ar_rs.at[mt], device_id={"tp": peer}, device_id_type=MESH
        )

    def ar_arrival(d):
        peer = lax.rem(mt + d, n_tp)
        return pltpu.make_async_remote_copy(
            ar_send, ar_recv.at[peer], ar_ss.at[0], ar_rs.at[peer], device_id={"tp": peer}, device_id_type=MESH
        )

    for d in range(1, n_tp):
        ar_copy(d).start()
    attention = ar_send[...].astype(F32)
    for d in range(1, n_tp):
        ar_arrival(d).wait_recv()
        attention = attention + ar_recv[lax.rem(mt + d, n_tp)].astype(F32)
    res = wide + attention
    for j in range(n_tp):
        residual[j] = res[:, j * cols:(j + 1) * cols]
    ffn = rms_scale(res, ffn_gain[...]).astype(BF16)
    gathered[0, me] = ffn[:, :half]
    gathered[1, me] = ffn[:, half:]

    def ag_piece(peer, s, send_sem):
        return pltpu.make_async_remote_copy(
            gathered.at[side, s], gathered.at[side, s], send_sem, ag_rs.at[s],
            device_id={"ep": peer}, device_id_type=MESH,
        )

    def ag_copy(k):
        peer = 2 * far_first(k) + inner
        return ag_piece(peer, me, ag_ss.at[0])

    def pair_copy(s):
        return ag_piece(across, s, ag_ss.at[0])

    def ag_arrival(s):
        return ag_piece(across, s, ag_ss.at[0])

    def fw_copy(s):
        return pltpu.make_async_remote_copy(
            gathered.at[side, s], gathered.at[side, s], fw_ss.at[0], fw_rs.at[s],
            device_id={"tp": partner}, device_id_type=MESH,
        )

    def fw_arrival(s):
        return pltpu.make_async_remote_copy(
            gathered.at[1 - side, s], gathered.at[1 - side, s], fw_ss.at[0], fw_rs.at[s],
            device_id={"tp": partner}, device_id_type=MESH,
        )

    pair_copy(me).start()

    @pl.loop(0, n_outer - 1)
    def _(k):
        ag_copy(k).start()

    for copy in dense_in:
        copy.wait()
    hidden = (silu(dot_nt(ffn, dg_v[...])) * dot_nt(ffn, du_v[...])).astype(BF16)
    logit = jnp.sum(hidden.astype(F32) * gate_vector[...], axis=-1, keepdims=True)
    l_send[...] = jnp.broadcast_to(logit, l_send.shape)
    @pl.loop(0, n_outer - 1)
    def _(k):
        s = 2 * near_first(k) + inner
        ag_arrival(s).wait_recv()
        pair_copy(s).start()
        fw_copy(s).start()

    for j in range(n_tp):
        dense_out_copies[j].wait()
        d_send[j] = dot(hidden, dd_v[j]).astype(BF16)

    def ds_copies(d):
        peer = lax.rem(mt + d, n_tp)
        return (
            pltpu.make_async_remote_copy(
                d_send.at[peer], d_recv.at[mt], ds_ss.at[0], ds_rs.at[mt],
                device_id={"tp": peer}, device_id_type=MESH,
            ),
            pltpu.make_async_remote_copy(
                l_send, l_recv.at[mt], lg_ss.at[0], lg_rs.at[mt], device_id={"tp": peer}, device_id_type=MESH
            ),
        )

    def ds_arrivals(d):
        peer = lax.rem(mt + d, n_tp)
        return (
            pltpu.make_async_remote_copy(
                d_send.at[peer], d_recv.at[peer], ds_ss.at[0], ds_rs.at[peer],
                device_id={"tp": peer}, device_id_type=MESH,
            ),
            pltpu.make_async_remote_copy(
                l_send, l_recv.at[peer], lg_ss.at[0], lg_rs.at[peer], device_id={"tp": peer}, device_id_type=MESH
            ),
        )

    for d in range(1, n_tp):
        for copy in ds_copies(d):
            copy.start()

    @pl.loop(0, n_outer)
    def _(k):
        o = jnp.where(k == 0, outer, near_first(jnp.maximum(k - 1, 0)))
        s = 2 * o + 1 - inner
        ag_arrival(s).wait_recv()
        fw_copy(s).start()

    for copy in expert_in:
        copy.wait()
    for copy in expert_out:
        copy.wait()

    @pl.loop(1, n_ep)
    def _(d):
        fw_arrival(lax.rem(me + n_ep - d, n_ep)).wait_recv()

    span = min(n_ep, 8)
    rows = span * n_seq

    @pl.loop(0, n_ep // span)
    def _(i):
        groups = pl.ds(i * span, span)
        low = gathered[0, groups].reshape(rows, half)
        high = gathered[1, groups].reshape(rows, half)
        pre = dot(low, wg_v[:half, :]) + dot(high, wg_v[half:, :])
        upper = dot(low, wu_v[:half, :]) + dot(high, wu_v[half:, :])
        act = (silu(pre) * upper).astype(BF16)
        for j in range(n_tp):
            p_send[j % 2, j // 2, groups] = dot(act, wd_v[j]).astype(BF16).reshape(span, n_seq, cols)

    def near_copy(x, g):
        return pltpu.make_async_remote_copy(
            p_send.at[1 - side, x, g], n_recv.at[x, g], p_ss.at[0], p_rs.at[x, g],
            device_id={"tp": partner}, device_id_type=MESH,
        )

    def far_copy(d, g):
        x = lax.rem(far + d, n_far)
        return pltpu.make_async_remote_copy(
            x_send.at[x, g], x_recv.at[far, g], x_ss.at[0], x_rs.at[far, g],
            device_id={"tp": 2 * x + side}, device_id_type=MESH,
        )

    def far_arrival(d, g):
        x = lax.rem(far + d, n_far)
        return pltpu.make_async_remote_copy(
            x_send.at[x, g], x_recv.at[x, g], x_ss.at[0], x_rs.at[x, g],
            device_id={"tp": 2 * x + side}, device_id_type=MESH,
        )

    def e_copy(g):
        return pltpu.make_async_remote_copy(
            e_send.at[g], e_recv.at[me], e_ss.at[0], e_rs.at[me], device_id={"ep": g}, device_id_type=MESH
        )

    def e_arrival(g):
        return pltpu.make_async_remote_copy(
            e_send.at[g], e_recv.at[g], e_ss.at[0], e_rs.at[g], device_id={"ep": g}, device_id_type=MESH
        )

    @pl.loop(0, n_ep)
    def _(k):
        g = group_at(k)
        for d in range(1, n_far + 1):
            near_copy(lax.rem(far + d, n_far), g).start()

    def pair_sum(x, g):
        near_copy(x, g).wait_recv()
        return p_send[side, x, g].astype(F32) + n_recv[x, g].astype(F32)

    @pl.loop(0, n_ep)
    def _(k):
        g = group_at(k)
        for d in range(1, n_far):
            x = lax.rem(far + d, n_far)
            x_send[x, g] = pair_sum(x, g).astype(BF16)
            far_copy(d, g).start()

    def summed(g):
        total = pair_sum(far, g)
        for d in range(1, n_far):
            far_arrival(d, g).wait_recv()
            total = total + x_recv[lax.rem(far + d, n_far), g].astype(F32)
        return total.astype(BF16)

    @pl.loop(0, n_ep - 1)
    def _(k):
        g = group_at(k)
        e_send[g] = summed(g)
        e_copy(g).start()

    e_recv[me] = summed(me)

    dense_sum = d_send[mt].astype(F32)
    logit_sum = l_send[...]
    for d in range(1, n_tp):
        for copy in ds_arrivals(d):
            copy.wait_recv()
        peer = lax.rem(mt + d, n_tp)
        dense_sum = dense_sum + d_recv[peer].astype(F32)
        logit_sum = logit_sum + l_recv[peer]
    gate = 1.0 / (1.0 + jnp.exp(-logit_sum[:, 0:1]))
    total = residual[mt] + gate * dense_sum

    eye = lax.broadcasted_iota(jnp.int32, (n_seq, n_seq), 0) == lax.broadcasted_iota(jnp.int32, (n_seq, n_seq), 1)

    def column(row):
        return jnp.sum(jnp.where(eye, row, 0.0), axis=1, keepdims=True)

    route_columns = [column(routes_t[k:k + 1, :].astype(F32)) for k in range(TOPK)]
    weight_columns = [column(weight_t[k:k + 1, :]) for k in range(TOPK)]

    def add_expert(e, acc):
        coef = jnp.zeros((n_seq, 1), F32)
        number = jnp.full((n_seq, 1), e, jnp.int32).astype(F32)
        for k in range(TOPK):
            coef = coef + jnp.where(route_columns[k] == number, weight_columns[k], 0.0)
        return acc + coef * e_recv[e].astype(F32)

    total = add_expert(me, total)

    def receive(d, acc):
        e = lax.rem(me + n_ep - d, n_ep)
        e_arrival(e).wait_recv()
        return add_expert(e, acc)

    total = lax.fori_loop(1, n_ep, receive, total)
    out[...] = total.astype(BF16)

    def drain(ref, sem):
        pltpu.make_async_copy(ref, ref, sem.at[0]).wait()

    drain(ar_recv.at[pl.ds(0, n_tp - 1)], ar_ss)
    drain(d_recv.at[pl.ds(0, n_tp - 1)], ds_ss)
    drain(l_recv.at[pl.ds(0, n_tp - 1)], lg_ss)
    drain(gathered.at[0, pl.ds(0, n_ep - 1)], ag_ss)
    drain(gathered.at[1, pl.ds(0, n_ep - 1)], fw_ss)
    drain(n_recv, p_ss)
    drain(x_send.at[pl.ds(0, n_far - 1)], x_ss)
    drain(e_send.at[pl.ds(0, n_ep - 1)], e_ss)


def shards(
    tokens, norm_gain, query_weight, key_weight, value_weight, output_weight, head_gain, lambdas,
    key_cache, value_cache, lengths, ffn_gain, routes, route_weight, expert_gate, expert_up,
    expert_down, dense_gate, dense_up, dense_down, gate_vector,
):
    n_ep, n_tp = lax.axis_size("ep"), lax.axis_size("tp")
    n_seq, width = tokens.shape
    cols = width // n_tp
    half = width // 2
    cache_len = key_cache.shape[1]
    keys = key_cache.reshape(n_seq, cache_len, 2 * DQK)
    values = value_cache.reshape(n_seq, cache_len, DV)
    hid = expert_gate.shape[2]
    dense = dense_gate.shape[0]
    vmem = pl.BlockSpec(memory_space=pltpu.VMEM)
    hbm = pl.BlockSpec(memory_space=pl.ANY)

    def held(*shape, dtype=BF16):
        return pltpu.VMEM(shape, dtype)

    def sems(*shape):
        return pltpu.SemaphoreType.DMA(shape)

    return pl.pallas_call(
        functools.partial(layer_kernel, n_ep, n_tp),
        out_shape=pltpu.VMEM((n_seq, cols), BF16),
        in_specs=[hbm] * 21,
        out_specs=vmem,
        scratch_shapes=[
            pltpu.SMEM(lengths.shape, jnp.int32), pltpu.SMEM(lambdas.shape, F32),
            held(n_seq, width), held(1, width, dtype=F32), held(1, head_gain.shape[0], dtype=F32),
            held(1, width, dtype=F32), held(1, dense, dtype=F32), held(TOPK, n_seq, dtype=jnp.int32),
            held(TOPK, n_seq, dtype=F32),
            held(*query_weight.shape), held(*key_weight.shape), held(*value_weight.shape), held(*output_weight.shape),
            held(*keys.shape), held(*values.shape),
            held(width, hid), held(width, hid), held(n_tp, hid, cols),
            held(dense, width), held(dense, width), held(n_tp, dense, cols),
            held(n_seq, 8, 2 * DQK, dtype=F32), held(n_seq, 1, 2 * DQK, dtype=F32),
            held(n_seq, 1, DV, dtype=F32), held(n_seq, 8, DV, dtype=F32),
            held(n_seq, width), held(n_tp, n_seq, width), held(n_tp, n_seq, cols, dtype=F32),
            held(2, n_ep, n_seq, half),
            held(n_tp, n_seq, cols), held(n_tp, n_seq, cols),
            held(n_seq, 128, dtype=F32), held(n_tp, n_seq, 128, dtype=F32),
            held(2, n_tp // 2, n_ep, n_seq, cols), held(n_tp // 2, n_ep, n_seq, cols),
            held(n_tp // 2, n_ep, n_seq, cols), held(n_tp // 2, n_ep, n_seq, cols),
            held(n_ep, n_seq, cols), held(n_ep, n_seq, cols),
            sems(9), sems(8 + 2 * n_tp), sems(2 * (n_seq // SEQ_CHUNK)),
            sems(1), sems(n_tp), sems(1), sems(n_ep), sems(1), sems(n_ep),
            sems(1), sems(n_tp), sems(1), sems(n_tp),
            sems(1), sems(n_tp // 2, n_ep), sems(1), sems(n_tp // 2, n_ep), sems(1), sems(n_ep),
        ],
        compiler_params=pltpu.CompilerParams(
            collective_id=0, has_side_effects=True, vmem_limit_bytes=58 * 1024 * 1024
        ),
    )(
        lengths, lambdas,
        tokens, norm_gain[None, :], head_gain[None, :], ffn_gain[None, :], gate_vector[None, :],
        routes.T, route_weight.T,
        query_weight, key_weight, value_weight, output_weight, keys, values,
        expert_gate[0], expert_up[0], expert_down[0], dense_gate, dense_up, dense_down,
    )


def solution(mesh):
    placed = (
        P("ep", None),
        P(),
        P(None, "tp"),
        P(None, "tp"),
        P(None, "tp"),
        P("tp", None),
        P(),
        P("tp"),
        P("ep", None, "tp", None),
        P("ep", None, "tp", None),
        P("ep"),
        P(),
        P("ep", None),
        P("ep", None),
        P("ep", None, "tp"),
        P("ep", None, "tp"),
        P("ep", "tp", None),
        P("tp", None),
        P("tp", None),
        P("tp", None),
        P("tp"),
    )
    return jax.shard_map(
        shards, mesh=mesh, in_specs=placed, out_specs=P("ep", "tp"), check_vma=False
    )
```
